32 devices in a mesh: sp: 4 (over z), fs: 4 (over y, x), tp: 2 (over core).
Axes of the slice: x: 2, y: 2, z: 4, core: 2. Of those that a mesh axis runs over, the one named last changes fastest.
Arguments:
- tokens: bfloat16 [1024, 2048], P(('sp', 'fs', 'tp')), may hold values from -6 to 6
- norm_gain: float32 [2048], replicated, may hold values from 0.1 to 1.9
- w_query: bfloat16 [2048, 1024], P(None, ('fs', 'tp')), may hold values from -0.125 to 0.125
- w_key: bfloat16 [2048, 1024], P(None, ('fs', 'tp')), may hold values from -0.125 to 0.125
- w_value: bfloat16 [2048, 1024], P(None, ('fs', 'tp')), may hold values from -0.125 to 0.125
- w_pool: bfloat16 [2048, 1024], P(None, ('fs', 'tp')), may hold values from -0.125 to 0.125
- query_gain: float32 [64], replicated, may hold values from 1.2 to 1.6
- key_gain: float32 [64], replicated, may hold values from 1.2 to 1.6
- lambdas: float32 [8], P(('fs', 'tp')), may hold values from 0.3 to 0.8
- head_gain: float32 [128], replicated, may hold values from 0.1 to 1.9
- w_out_attn: bfloat16 [1024, 2048], P(('fs', 'tp')), may hold values from -0.125 to 0.125
- w_out_pool: bfloat16 [1024, 2048], P(('fs', 'tp')), may hold values from -0.125 to 0.125
Outputs:
- layer_out: bfloat16 [1024, 2048], P(('sp', 'fs', 'tp'))
The draws below stay inside these ranges and needn't reach their ends.
All inputs are finite; a program needn't handle non-finite values.
Results may differ from the reference program's by a relative error of at most 0.015.
Values may be sent and summed in bfloat16 or wider, within the bound.
A program may use at most 128 MiB of HBM per device.

```python
import math
import jax
import jax.numpy as jnp
from jax import lax

D = 2048
HEADS = 8
HEAD_DIM = 64
V_DIM = 128
ATTN_WIDTH = 1024
POOL_GROUPS = 4
POOL_GROUP_DIM = 256
POOL_WIDTH = 1024
SEQ = 1024


def block_scale(rng, shape, cuts, low, high):
    def one(axis_at, blocks):
        steps = jax.random.uniform(jax.random.fold_in(jax.random.fold_in(rng, 6), axis_at), (blocks,), jnp.float32, low / len(cuts), high / len(cuts))
        return jnp.repeat(jnp.exp(steps), shape[axis_at] // blocks).reshape((-1,) + (1,) * (len(shape) - axis_at - 1))

    level = one(*cuts[0])
    for cut in cuts[1:]:
        level = level * one(*cut)
    return level


def scatter_about(key, extent, spread, most, split=(), kind=jnp.bfloat16):
    entries = spread * jax.random.normal(key, extent, jnp.float32)
    if split:
        entries = entries * block_scale(key, extent, split, -0.22, 0.18)
    return jnp.clip(entries, -most, most).astype(kind)


def setup_inputs(seed: int = 0) -> dict:
    key_list = jax.random.split(jax.random.key(seed), 13)
    return {
        "tokens": scatter_about(key_list[0], (SEQ, D), 1.0, 6.0, ((0, 32),)),
        "norm_gain": jnp.clip(1.0 + 0.18 * jax.random.normal(key_list[1], (D,), jnp.float32), 0.1, 1.9),
        "w_query": scatter_about(key_list[2], (D, HEADS * 2 * HEAD_DIM), D ** -0.5, 0.125, ((1, 8),)),
        "w_key": scatter_about(key_list[3], (D, HEADS * 2 * HEAD_DIM), D ** -0.5, 0.125, ((1, 8),)),
        "w_value": scatter_about(key_list[4], (D, ATTN_WIDTH), D ** -0.5, 0.125, ((1, 8),)),
        "w_pool": scatter_about(key_list[5], (D, POOL_WIDTH), D ** -0.5, 0.125, ((1, 8),)),
        "query_gain": jnp.clip(jax.random.uniform(key_list[6], (HEAD_DIM,), jnp.float32, 1.2, 1.6), 1.2, 1.6),
        "key_gain": jnp.clip(jax.random.uniform(key_list[7], (HEAD_DIM,), jnp.float32, 1.2, 1.6), 1.2, 1.6),
        "lambdas": jnp.clip(0.3 + 0.5 * jax.random.uniform(key_list[8], (HEADS,), jnp.float32) ** block_scale(key_list[8], (HEADS,), ((0, 8),), -0.2, 0.2), 0.3, 0.8),
        "head_gain": jnp.clip(1.0 + 0.18 * jax.random.normal(key_list[9], (V_DIM,), jnp.float32), 0.1, 1.9),
        "w_out_attn": scatter_about(key_list[10], (ATTN_WIDTH, D), (ATTN_WIDTH + POOL_WIDTH) ** -0.5, 0.125, ((0, 8),)),
        "w_out_pool": scatter_about(key_list[11], (POOL_WIDTH, D), (ATTN_WIDTH + POOL_WIDTH) ** -0.5, 0.125, ((0, 8),)),
    }


epsilon = 1e-06
windows = (2, 4, 8, 16)

def rms_scale(values, gain):
    return values * lax.rsqrt(lax.optimization_barrier(jnp.mean(values * values, axis=-1, keepdims=True)) + epsilon) * gain

def attend_head(queries, keys, values, lam_one):
    query_block = math.gcd(SEQ, 512)
    score_scale = HEAD_DIM ** (-0.5)
    key_pos = jnp.arange(SEQ, dtype=jnp.int32)
    keys32 = keys.astype(jnp.float32)
    values32 = values.astype(jnp.float32)
    blocked = queries.reshape(SEQ // query_block, query_block, 2, HEAD_DIM)
    starts = (jnp.arange(SEQ // query_block, dtype=jnp.int32) * query_block).astype(jnp.int32)

    def one_block(inputs):
        query_rows, first_row = inputs
        scores = jnp.einsum('qcd,kcd->cqk', query_rows.astype(jnp.float32), keys32) * score_scale
        query_pos = first_row + jnp.arange(query_block, dtype=jnp.int32)
        visible = key_pos[None, :] <= query_pos[:, None]
        expo = jnp.where(visible[None], jnp.exp(scores), 0.0)
        totals = lax.optimization_barrier(jnp.sum(expo, axis=-1))
        rounded = lax.optimization_barrier(expo.astype(jnp.bfloat16))
        numer = jnp.einsum('cqk,ke->cqe', rounded.astype(jnp.float32), values32)
        return numer[0] / totals[0][:, None] - lam_one * numer[1] / totals[1][:, None]
    head_out = lax.map(one_block, (blocked, starts))
    return head_out.reshape(SEQ, V_DIM)

def pool_mix(pool_input):
    source = pool_input.astype(jnp.float32).reshape(SEQ, POOL_GROUPS, POOL_GROUP_DIM)
    positions = jnp.arange(SEQ, dtype=jnp.float32)
    outputs = []
    for group_index, width_g in enumerate(windows):
        channel = source[:, group_index]
        window_sum = channel
        for offset in range(1, width_g):
            earlier = jnp.concatenate([jnp.zeros((offset, POOL_GROUP_DIM), jnp.float32), channel[:SEQ - offset]], axis=0)
            window_sum = window_sum + earlier
        divisor = jnp.minimum(positions + 1.0, float(width_g))[:, None]
        outputs.append(window_sum / divisor - channel)
    return jnp.stack(outputs, axis=1).reshape(SEQ, POOL_WIDTH).astype(jnp.bfloat16)

def reference(tokens, norm_gain, w_query, w_key, w_value, w_pool, query_gain, key_gain, lambdas, head_gain, w_out_attn, w_out_pool):
    normed = rms_scale(tokens.astype(jnp.float32), norm_gain).astype(jnp.bfloat16)
    query_raw = jnp.dot(normed, w_query, preferred_element_type=jnp.float32).reshape(SEQ, HEADS, 2, HEAD_DIM)
    queries = rms_scale(query_raw, query_gain).astype(jnp.bfloat16)
    key_raw = jnp.dot(normed, w_key, preferred_element_type=jnp.float32).reshape(SEQ, HEADS, 2, HEAD_DIM)
    keys = rms_scale(key_raw, key_gain).astype(jnp.bfloat16)
    values = jnp.dot(normed, w_value, preferred_element_type=jnp.float32).astype(jnp.bfloat16).reshape(SEQ, HEADS, V_DIM)
    pool_input = jnp.dot(normed, w_pool, preferred_element_type=jnp.float32).astype(jnp.bfloat16)

    def per_head(inputs):
        query_h, key_h, value_h, lam_h = inputs
        head_out = attend_head(query_h, key_h, value_h, lam_h)
        return rms_scale(head_out, head_gain).astype(jnp.bfloat16)
    attended = lax.map(per_head, (jnp.transpose(queries, (1, 0, 2, 3)), jnp.transpose(keys, (1, 0, 2, 3)), jnp.transpose(values, (1, 0, 2)), lambdas))
    attended = jnp.transpose(attended, (1, 0, 2)).reshape(SEQ, HEADS * V_DIM)
    pooled = pool_mix(pool_input)
    summed = jnp.dot(attended, w_out_attn, preferred_element_type=jnp.float32) + jnp.dot(pooled, w_out_pool, preferred_element_type=jnp.float32)
    return summed.astype(jnp.bfloat16)
```

```python
import functools

import jax
import jax.numpy as jnp
from jax import lax
from jax.experimental import pallas as pl
from jax.experimental.pallas import tpu as pltpu
from jax.sharding import PartitionSpec as P

HEAD_DIM = 64
POOL_GROUP_DIM = 256
HALO = 16
EPS = 1e-06
MESH = pl.DeviceIdType.MESH
F32 = jnp.float32
BF16 = jnp.bfloat16


def kernel(
    n_sp, n_fs, col_chunks,
    tokens_hbm, norm_gain_hbm, wq_hbm, wk_hbm, wv_hbm, wp_hbm, query_gain_hbm, key_gain_hbm,
    lambdas_hbm, head_gain_hbm, woa_hbm, wop_hbm,
    out_ref,
    norm_gain_ref, query_gain_ref, key_gain_ref, lambdas_ref, head_gain_ref,
    tok, gathered, win, wout, kv, qhat, pin, halo_src, halo, numer, total, merged,
    part_send, part_recv, chip_own, chip_send, chip_relay, chip_recv,
    small_sem, tok_sem, win_sem, wout_sem, send_sem, ag_recv, fwd_recv, kv_send, kv_recv,
    halo_send, halo_recv, a_recv, b_recv,
):
    s = lax.axis_index("sp")
    f = lax.axis_index("fs")
    t = lax.axis_index("tp")
    mate = (s, f, 1 - t)
    rows, width = tok.shape
    chip_rows = 2 * rows
    own_rows = n_fs * chip_rows
    heads = lambdas_ref.shape[1]
    qc = wq_hbm.shape[1]
    vc = wv_hbm.shape[1]
    pc = wp_hbm.shape[1]
    v_dim = head_gain_ref.shape[1]
    pair = 2 * HEAD_DIM

    def peer(k):
        return lax.rem(f + k, n_fs)

    fx = f + 1 - 2 * lax.rem(f, 2)
    fy = lax.rem(f + 2, n_fs)
    chips = (f, fx, fy, lax.rem(fx + 2, n_fs))

    tok_copy = pltpu.make_async_copy(tokens_hbm, tok, tok_sem)
    tok_copy.start()
    barrier = pltpu.get_barrier_semaphore()
    pl.semaphore_signal(barrier, inc=1, device_id=mate, device_id_type=MESH)
    for chip in (fx, fy):
        pl.semaphore_signal(barrier, inc=1, device_id=(s, chip, t), device_id_type=MESH)

    @pl.when(s > 0)
    def _():
        pl.semaphore_signal(barrier, inc=1, device_id=(s - 1, f, t), device_id_type=MESH)

    @pl.when(s < n_sp - 1)
    def _():
        pl.semaphore_signal(barrier, inc=1, device_id=(s + 1, f, t), device_id_type=MESH)

    small_copies = [
        pltpu.make_async_copy(src, dst, small_sem.at[i])
        for i, (src, dst) in enumerate((
            (norm_gain_hbm, norm_gain_ref), (query_gain_hbm, query_gain_ref),
            (key_gain_hbm, key_gain_ref), (lambdas_hbm, lambdas_ref),
            (head_gain_hbm, head_gain_ref),
        ))
    ]
    for c in small_copies:
        c.start()
    win_copies = []
    at = 0
    for w, c in ((wk_hbm, qc), (wv_hbm, vc), (wq_hbm, qc), (wp_hbm, pc)):
        win_copies.append(pltpu.make_async_copy(w, win.at[:, pl.ds(at, c)], win_sem))
        at += c
    wout_copies = [
        pltpu.make_async_copy(woa_hbm, wout.at[pl.ds(0, vc), :], wout_sem),
        pltpu.make_async_copy(wop_hbm, wout.at[pl.ds(vc, pc), :], wout_sem),
    ]
    for c in win_copies + wout_copies:
        c.start()

    small_copies[0].wait()
    tok_copy.wait()
    x = tok[...].astype(F32)
    x = x * lax.rsqrt(jnp.mean(x * x, axis=-1, keepdims=True) + EPS) * norm_gain_ref[...]
    gathered[f, t] = x.astype(BF16).reshape(2, rows // 2, width)

    pl.semaphore_wait(
        barrier, 3 + jnp.where(s > 0, 1, 0) + jnp.where(s < n_sp - 1, 1, 0)
    )

    def along(way, i, chip, half):
        slot = gathered.at[chip, t, half]
        return pltpu.make_async_remote_copy(
            slot, slot, send_sem, ag_recv.at[way, i],
            device_id=(s, (fx, fy)[way], t), device_id_type=MESH,
        )

    own = [[along(way, half, f, half) for half in range(2)] for way in range(2)]
    for way, half in ((0, 1), (1, 0), (0, 0), (1, 1)):
        own[way][half].start()
    far = [along(0, 2, fy, 0), along(1, 2, fx, 1)]

    def across(k, half):
        slot = gathered.at[chips[k], t, half]
        return pltpu.make_async_remote_copy(
            slot, slot, send_sem, fwd_recv.at[k, half],
            device_id=mate, device_id_type=MESH,
        )

    forwards = [[across(k, half) for half in range(2)] for k in range(n_fs)]
    for c in forwards[0]:
        c.start()

    lane = lax.broadcasted_iota(jnp.int32, (chip_rows, pair), 1)
    low = lane < HEAD_DIM

    def norm_pair(raw, gain):
        sq = raw * raw
        first = jnp.sum(jnp.where(low, sq, 0.0), axis=-1, keepdims=True) * (1.0 / HEAD_DIM)
        second = jnp.sum(jnp.where(low, 0.0, sq), axis=-1, keepdims=True) * (1.0 / HEAD_DIM)
        return raw * jnp.where(low, lax.rsqrt(first + EPS), lax.rsqrt(second + EPS)) * gain

    for c in small_copies[1:]:
        c.wait()
    qg = jnp.concatenate([query_gain_ref[...]] * 2, axis=1)
    kg = jnp.concatenate([key_gain_ref[...]] * 2, axis=1)

    last = n_fs - 1

    def kv_copy(j, k):
        slot = kv.at[j, chips[k]]
        return pltpu.make_async_remote_copy(
            slot, slot, kv_send.at[j], kv_recv.at[j, k],
            device_id=(s + 1, f, t), device_id_type=MESH,
        )

    def relay(d, k):
        @pl.when(s >= d)
        def _():
            c = kv_copy(s - d, k)
            c.wait_recv()

            @pl.when(s < n_sp - 1)
            def _():
                c.start()

    for k in range(n_fs):
        chip = chips[k]
        if k == 1:
            own[1][0].wait_recv()
            far[0].start()
            forwards[2][0].start()
            own[0][1].wait_recv()
            far[1].start()
            forwards[1][1].start()
            own[0][0].wait_recv()
            forwards[1][0].start()
            own[1][1].wait_recv()
            forwards[2][1].start()
        if k == last:
            for half in range(2):
                far[half].wait_recv()
                forwards[last][half].start()
            relay(1, 0)
        for c in forwards[k]:
            c.wait_recv()
        if k == 0:
            pltpu.make_async_copy(win, win, win_sem).wait()
        block = gathered[chip].reshape(chip_rows, width)
        proj = jnp.dot(block, win[:, : qc + vc], preferred_element_type=F32)
        for h in range(heads):
            kv[s, chip, :, h * pair : (h + 1) * pair] = norm_pair(
                proj[:, h * pair : (h + 1) * pair], kg
            ).astype(BF16)
        kv[s, chip, :, qc : qc + vc] = proj[:, qc : qc + vc].astype(BF16)

        @pl.when(s < n_sp - 1)
        def _(k=k):
            kv_copy(s, k).start()

        proj = jnp.dot(block, win[:, qc + vc :], preferred_element_type=F32)
        for h in range(heads):
            at = h * pair
            q = norm_pair(proj[:, at : at + pair], qg)
            q = q.astype(BF16).astype(F32) * HEAD_DIM ** (-0.5)
            qhat[h, 0, chip] = jnp.where(low, q, 0.0).astype(BF16)
            qhat[h, 1, chip] = jnp.where(low, 0.0, q).astype(BF16)
        pin[chip] = proj[:, qc:].astype(BF16).astype(F32)

    halo_src[...] = pin[n_fs - 1, chip_rows - HALO :, :].astype(BF16)
    halo_copy = pltpu.make_async_remote_copy(
        halo_src, halo, halo_send, halo_recv, device_id=(s + 1, f, t), device_id_type=MESH,
    )

    @pl.when(s < n_sp - 1)
    def _():
        halo_copy.start()

    def fold(p):
        acc = p[:, :128]
        for i in range(1, p.shape[1] // 128):
            acc = acc + p[:, i * 128 : (i + 1) * 128]
        return acc

    def attend(j, diagonal):
        for h in range(heads):
            keys = kv[j, :, :, h * pair : (h + 1) * pair].reshape(own_rows, pair)
            vals = kv[j, :, :, qc + h * v_dim : qc + (h + 1) * v_dim].reshape(own_rows, v_dim)
            for c in range(2):
                q = qhat[h, c].reshape(own_rows, pair)
                p = jnp.exp(
                    lax.dot_general(q, keys, (((1,), (1,)), ((), ())), preferred_element_type=F32)
                )
                if diagonal:
                    r = lax.broadcasted_iota(jnp.int32, p.shape, 0)
                    col = lax.broadcasted_iota(jnp.int32, p.shape, 1)
                    p = jnp.where(col <= r, p, 0.0)
                pv = jnp.dot(p.astype(BF16), vals, preferred_element_type=F32)
                if diagonal:
                    numer[h, c] = pv
                    total[h, c] = fold(p)
                else:
                    numer[h, c] += pv
                    total[h, c] += fold(p)

    relay(1, 1)
    relay(1, 2)
    relay(2, 0)
    attend(s, True)
    relay(2, 1)
    relay(3, 0)

    @pl.when(s > 0)
    def _():
        halo_copy.wait_recv()

    @pl.when(s == 0)
    def _():
        halo[...] = jnp.zeros_like(halo)

    group = ((f * 2 + t) * pc) // POOL_GROUP_DIM
    ext = jnp.concatenate([halo[...].astype(F32), pin[...].reshape(own_rows, pc)], axis=0)
    gvec = jnp.full(ext.shape, group, jnp.int32)
    window = ext + pltpu.roll(ext, 1, 0)
    chosen = window
    for i, shift in enumerate((2, 4, 8)):
        window = window + pltpu.roll(window, shift, 0)
        chosen = jnp.where(gvec > i, window, chosen)
    chosen = chosen[HALO:]
    pos = s * own_rows + lax.broadcasted_iota(jnp.int32, (own_rows, pc), 0)
    size = jnp.left_shift(jnp.full((own_rows, pc), 2, jnp.int32), gvec[HALO:])
    divisor = jnp.minimum(pos + 1, size).astype(F32)
    pooled = (chosen / divisor - ext[HALO:]).astype(BF16)
    merged[:, :, :, vc:] = pooled.reshape(n_fs, 2, rows, pc)

    def earlier(d, carry):
        j = s - d
        for k in range(last, -1, -1):
            relay(d + last - k, k)
        attend(j, False)
        return carry

    lax.fori_loop(1, s + 1, earlier, 0)

    for h in range(heads):
        first = numer[h, 0] / jnp.sum(total[h, 0], axis=-1, keepdims=True)
        second = numer[h, 1] / jnp.sum(total[h, 1], axis=-1, keepdims=True)
        o = first - lambdas_ref[0, h] * second
        o = o * lax.rsqrt(jnp.mean(o * o, axis=-1, keepdims=True) + EPS) * head_gain_ref[...]
        merged[:, :, :, h * v_dim : (h + 1) * v_dim] = o.astype(BF16).reshape(
            n_fs, 2, rows, v_dim
        )

    pltpu.make_async_copy(wout, wout, wout_sem).wait()
    depth = vc + pc
    cw = out_ref.shape[1] // col_chunks
    theirs = merged[:, 1 - t].reshape(n_fs * rows, depth)
    mine = merged[:, t].reshape(n_fs * rows, depth)
    a_copies = []
    for n in range(col_chunks):
        y = jnp.dot(theirs, wout[:, n * cw : (n + 1) * cw], preferred_element_type=F32)
        part_send[n] = y.astype(BF16)
        c = pltpu.make_async_remote_copy(
            part_send.at[n], part_recv.at[n], send_sem, a_recv.at[n],
            device_id=mate, device_id_type=MESH,
        )
        c.start()
        a_copies.append(c)
    b_copies = []
    for n in range(col_chunks):
        y = jnp.dot(mine, wout[:, n * cw : (n + 1) * cw], preferred_element_type=F32)
        a_copies[n].wait_recv()
        y = y + part_recv[n].astype(F32)
        chip_own[n] = y.reshape(n_fs, rows, cw)
        chip_send[n] = y.astype(BF16).reshape(n_fs, rows, cw)
        near = chips[1 + n % 2]
        steps = []
        for i, (ref, to) in enumerate((
            (chip_send.at[n, chips[last]], near),
            (chip_send.at[n, near], near),
            (chip_relay.at[n], chips[2 - n % 2]),
        )):
            steps.append(pltpu.make_async_remote_copy(
                ref, chip_recv.at[n, i], send_sem, b_recv.at[n, i],
                device_id=(s, to, t), device_id_type=MESH,
            ))
        steps[0].start()
        steps[1].start()
        b_copies.append(steps)
    for n in range(col_chunks):
        b_copies[n][0].wait_recv()
        y = chip_own[n, chips[2 - n % 2]] + chip_recv[n, 0].astype(F32)
        chip_relay[n] = y.astype(BF16)
        b_copies[n][2].start()
    for n in range(col_chunks):
        b_copies[n][1].wait_recv()
        y = chip_own[n, f] + chip_recv[n, 1].astype(F32)
        b_copies[n][2].wait_recv()
        out_ref[:, n * cw : (n + 1) * cw] = (y + chip_recv[n, 2].astype(F32)).astype(BF16)

    sent = (len(own[0] + own[1] + far) + 2 * n_fs) * (rows // 2) * width
    sent += (col_chunks * n_fs + col_chunks * 3) * rows * cw
    depth_words = win.shape[1]
    assert sent % depth_words == 0 and sent // depth_words <= width
    drained = win.at[pl.ds(0, sent // depth_words), :]
    pltpu.make_async_copy(drained, drained, send_sem).wait()

    @pl.when(s < n_sp - 1)
    def _():
        halo_copy.wait_send()

        def drain(j, carry):
            pltpu.make_async_copy(kv.at[j], kv.at[j], kv_send.at[j]).wait()
            return carry

        lax.fori_loop(0, s + 1, drain, 0)


def solution(mesh):
    n_sp, n_fs, n_tp = mesh.shape["sp"], mesh.shape["fs"], mesh.shape["tp"]
    assert n_tp == 2 and n_fs == 4

    def body(tokens, norm_gain, w_query, w_key, w_value, w_pool, query_gain, key_gain,
             lambdas, head_gain, w_out_attn, w_out_pool):
        rows, width = tokens.shape
        out_width = w_out_attn.shape[1]
        heads = lambdas.shape[0]
        qc, vc, pc = w_query.shape[1], w_value.shape[1], w_pool.shape[1]
        v_dim = head_gain.shape[0]
        chip_rows = 2 * rows
        own_rows = n_fs * chip_rows
        col_chunks = 4
        cw = out_width // col_chunks
        hbm = pl.BlockSpec(memory_space=pl.ANY)
        vmem = pl.BlockSpec(memory_space=pltpu.VMEM)
        dma = pltpu.SemaphoreType.DMA
        return pl.pallas_call(
            functools.partial(kernel, n_sp, n_fs, col_chunks),
            out_shape=pltpu.VMEM((rows, out_width), BF16),
            in_specs=[hbm] * 12,
            out_specs=vmem,
            scratch_shapes=[
                pltpu.VMEM((1, width), F32),
                pltpu.VMEM((1, HEAD_DIM), F32),
                pltpu.VMEM((1, HEAD_DIM), F32),
                pltpu.SMEM((1, heads), F32),
                pltpu.VMEM((1, v_dim), F32),
                pltpu.VMEM((rows, width), BF16),
                pltpu.VMEM((n_fs, 2, 2, rows // 2, width), BF16),
                pltpu.VMEM((width, 2 * qc + vc + pc), BF16),
                pltpu.VMEM((vc + pc, out_width), BF16),
                pltpu.VMEM((n_sp, n_fs, chip_rows, qc + vc), BF16),
                pltpu.VMEM((heads, 2, n_fs, chip_rows, 2 * HEAD_DIM), BF16),
                pltpu.VMEM((n_fs, chip_rows, pc), F32),
                pltpu.VMEM((HALO, pc), BF16),
                pltpu.VMEM((HALO, pc), BF16),
                pltpu.VMEM((heads, 2, own_rows, v_dim), F32),
                pltpu.VMEM((heads, 2, own_rows, 128), F32),
                pltpu.VMEM((n_fs, 2, rows, vc + pc), BF16),
                pltpu.VMEM((col_chunks, n_fs * rows, cw), BF16),
                pltpu.VMEM((col_chunks, n_fs * rows, cw), BF16),
                pltpu.VMEM((col_chunks, n_fs, rows, cw), F32),
                pltpu.VMEM((col_chunks, n_fs, rows, cw), BF16),
                pltpu.VMEM((col_chunks, rows, cw), BF16),
                pltpu.VMEM((col_chunks, 3, rows, cw), BF16),
                dma((5,)), dma(()), dma(()), dma(()), dma(()),
                dma((2, 3)), dma((n_fs, 2)),
                dma((n_sp,)), dma((n_sp, n_fs)),
                dma(()), dma(()),
                dma((col_chunks,)), dma((col_chunks, 3)),
            ],
            compiler_params=pltpu.CompilerParams(
                collective_id=0, has_side_effects=True, vmem_limit_bytes=60 * 1024 * 1024
            ),
        )(tokens, norm_gain.reshape(1, -1), w_query, w_key, w_value, w_pool,
          query_gain.reshape(1, -1), key_gain.reshape(1, -1), lambdas.reshape(1, -1),
          head_gain.reshape(1, -1), w_out_attn, w_out_pool)

    cols = P(None, ("fs", "tp"))
    flat = P(("fs", "tp"), None)
    return jax.shard_map(
        body,
        mesh=mesh,
        in_specs=(P(("sp", "fs", "tp"), None), P(), cols, cols, cols, cols, P(), P(),
                  P(("fs", "tp")), P(), flat, flat),
        out_specs=P(("sp", "fs", "tp"), None),
        check_vma=False,
    )
```
